1024 devices in a mesh: ra: 16 (over z), cb: 8 (over y), dp: 8 (over x, core).
Axes of the slice: x: 4, y: 8, z: 16, core: 2. Of those that a mesh axis runs over, the one named last changes fastest.
Arguments:
- stream: bfloat16 [2048, 2048], P('dp', 'ra'), may hold values from -60 to 60
- norm_gain: float32 [2, 2048], P(None, 'ra'), may hold values from 0.1 to 1.9
- gate_weight: float32 [2, 2048, 5504], P(None, 'ra', 'cb'), may hold values from -0.125 to 0.125
- up_weight: float32 [2, 2048, 5504], P(None, 'ra', 'cb'), may hold values from -0.125 to 0.125
- down_weight: float32 [2, 5504, 2048], P(None, 'cb', 'ra'), may hold values from -0.078125 to 0.078125
- gate_scale: float32 [2, 5504], P(None, 'cb'), may hold values from 0.5 to 2
- up_scale: float32 [2, 5504], P(None, 'cb'), may hold values from 0.5 to 2
- down_scale: float32 [2, 2048], P(None, 'ra'), may hold values from 0.5 to 2
Outputs:
- result: bfloat16 [2048, 2048], P('dp', 'ra')
The draws below stay inside these ranges and needn't reach their ends.
All inputs are finite; a program needn't handle non-finite values.
Results may differ from the reference program's by a relative error of at most 0.04.
Values may be sent and summed in bfloat16 or wider, within the bound.
A program may use at most 32 MiB of HBM per device.

```python
import math
import jax
import jax.numpy as jnp
from jax import lax

D = 2048
FF = 5504
TOKENS = 2048
N_RA = 16


def draw_stream(key, part):
    keys = jax.random.split(jax.random.fold_in(key, 11), 3)
    position = jnp.arange(D).astype(jnp.float32) / D
    column_scale = 0.3 * 10.0 ** position * jax.random.uniform(keys[0], (D,), jnp.float32, 0.7, 1.4)
    row_scale = 10.0 ** jax.random.uniform(keys[1], (TOKENS, 1), jnp.float32, -0.5, 0.5)
    base = jnp.clip(jax.random.normal(keys[2], (TOKENS, D), jnp.float32), -4.0, 4.0)
    return (base * row_scale * column_scale).astype(jnp.bfloat16)


def level_of(key, dims, cuts, low, largest):
    level = 1.0
    for dim, blocks in cuts:
        heights = jax.random.uniform(jax.random.fold_in(jax.random.fold_in(key, 6), dim), (blocks,), jnp.float32, low / len(cuts), largest / len(cuts))
        level = level * jnp.repeat(jnp.exp(heights), dims[dim] // blocks).reshape((-1,) + (1,) * (len(dims) - 1 - dim))
    return level


def centred(rng, shape, scale, reach, shards=(), dtype=jnp.bfloat16):
    loudness = level_of(rng, shape, shards, -0.22, 0.18) if shards else 1.0
    drawn = jax.random.normal(rng, shape, jnp.float32) * scale * loudness
    return jnp.minimum(jnp.maximum(drawn, -reach), reach).astype(dtype)


def setup_inputs(seed: int = 0) -> dict:
    splits = jax.random.split(jax.random.key(seed), 9)
    stream = draw_stream(jax.random.fold_in(splits[8], 71), 0)
    norm_gain = jnp.clip(1.0 + 0.18 * jax.random.normal(splits[1], (2, D), jnp.float32), 0.1, 1.9)
    gate_weight = centred(splits[2], (2, D, FF), D ** -0.5, 0.125, ((1, 16), (2, 8)), jnp.float32)
    up_weight = centred(splits[3], (2, D, FF), D ** -0.5, 0.125, ((1, 16), (2, 8)), jnp.float32)
    down_weight = centred(splits[4], (2, FF, D), FF ** -0.5, 0.078125, ((1, 8), (2, 16)), jnp.float32)
    gate_scale = jnp.clip(jnp.exp(math.log(2.0) - 1.3862944 * jax.random.uniform(splits[5], (2, FF), jnp.float32) ** level_of(splits[5], (2, FF), ((1, 8),), -0.2, 0.2)), 0.5, 2.0)
    up_scale = jnp.clip(jnp.exp(math.log(2.0) - 1.3862944 * jax.random.uniform(splits[6], (2, FF), jnp.float32) ** level_of(splits[6], (2, FF), ((1, 8),), -0.2, 0.2)), 0.5, 2.0)
    down_scale = jnp.clip(jnp.exp(math.log(2.0) - 1.3862944 * jax.random.uniform(splits[7], (2, D), jnp.float32) ** level_of(splits[7], (2, D), ((1, 16),), -0.2, 0.2)), 0.5, 2.0)
    return {"stream": stream, "norm_gain": norm_gain, "gate_weight": gate_weight, "up_weight": up_weight, "down_weight": down_weight, "gate_scale": gate_scale, "up_scale": up_scale, "down_scale": down_scale}


epsilon = 1e-06
residual_scale = 0.5

def block_sums(normed, weight):
    width = D // N_RA

    def add_block(carry, index):
        start = (index * width).astype(jnp.int32)
        columns = lax.dynamic_slice_in_dim(normed, start, width, 1)
        rows = lax.dynamic_slice_in_dim(weight, start, width, 0)
        piece = jnp.dot(columns, rows, preferred_element_type=jnp.float32).astype(jnp.bfloat16)
        piece = lax.optimization_barrier(piece)
        return (carry + piece.astype(jnp.float32), None)
    initial = jnp.zeros((normed.shape[0], weight.shape[1]), jnp.float32)
    total, unused = lax.scan(add_block, initial, jnp.arange(N_RA).astype(jnp.int32))
    return total

def half_step(stream, gain, gate_weight, up_weight, down_weight, gate_scale, up_scale, down_scale):
    widened = stream.astype(jnp.float32)
    squares = lax.optimization_barrier(jnp.sum(widened * widened, axis=1, keepdims=True))
    inverse = lax.rsqrt(squares / D + epsilon)
    normed = (widened * gain).astype(jnp.bfloat16)
    gate_sum = block_sums(normed, gate_weight.astype(jnp.bfloat16)) * inverse * gate_scale
    up_sum = block_sums(normed, up_weight.astype(jnp.bfloat16)) * inverse * up_scale
    hidden = (jax.nn.silu(gate_sum) * up_sum).astype(jnp.bfloat16)
    branch = jnp.dot(hidden, down_weight.astype(jnp.bfloat16), preferred_element_type=jnp.float32) * down_scale
    return (residual_scale * widened + branch).astype(jnp.bfloat16)

def reference(stream, norm_gain, gate_weight, up_weight, down_weight, gate_scale, up_scale, down_scale):
    current = stream
    for block_index in range(2):
        current = half_step(current, norm_gain[block_index], gate_weight[block_index], up_weight[block_index], down_weight[block_index], gate_scale[block_index], up_scale[block_index], down_scale[block_index])
    return current
```

```python
import functools

import jax
import jax.numpy as jnp
from jax import lax
from jax.experimental import pallas as pl
from jax.experimental.pallas import tpu as pltpu
from jax.sharding import PartitionSpec as P

MESH = pl.DeviceIdType.MESH
D = 2048
epsilon = 1e-06
residual_scale = 0.5

NZ, NY = 16, 8
ROWS = 32
TILE = 16
QUAD = (0, 1, 3, 2)
F32, BF16 = jnp.float32, jnp.bfloat16


def kernel(
    stream, gain, gate, up, down, gate_scale, up_scale, down_scale, out,
    xin, gain_v, gate_v, up_v, down_v, gs_v, us_v, ds_v,
    parts, w0, w1, xg, ob, rb, yb,
    in_sem, a_send, y_send, x_send, d_send, a_recv, y_recv, x_recv, d_recv,
    s_send, s_recv, o_send, o_recv, f_send, f_recv,
):
    z, y, d = lax.axis_index("ra"), lax.axis_index("cb"), lax.axis_index("dp")
    zq, zl = z // 4, z % 4
    x, c = d // 2, d % 2
    p = x % 2
    own = 2 * c + p
    classes = (own, 2 * c + 1 - p, 2 * (1 - c) + p, 2 * (1 - c) + 1 - p)
    weights = (w0, w1)

    def at_z(quad, low):
        return {"ra": 4 * ((zq + quad) % 4) + (zl + low) % 4}

    far_z = sorted(
        [(k, min(k, NZ - k)) for k in range(1, NZ)], key=lambda t: -t[1]
    )
    z_peers = [k for k, _ in far_z]
    y_plus, y_minus = {"cb": (y + 1) % NY}, {"cb": (y + NY - 1) % NY}
    x_plus, x_minus = {"dp": (d + 2) % 8}, {"dp": (d + 6) % 8}
    partner = {"dp": d + 1 - 2 * c}

    barrier = pltpu.get_barrier_semaphore()
    for k in z_peers:
        pl.semaphore_signal(barrier, 1, device_id={"ra": (z + k) % NZ}, device_id_type=MESH)
    for k in (4, 3, 5, 2, 6, 1, 7):
        pl.semaphore_signal(barrier, 1, device_id={"cb": (y + k) % NY}, device_id_type=MESH)
    for peer in (x_plus, x_minus, partner):
        pl.semaphore_signal(barrier, 1, device_id=peer, device_id_type=MESH)

    loads = [
        pltpu.make_async_copy(src, dst, in_sem.at[i])
        for i, (src, dst) in enumerate([
            (gate_scale, gs_v), (up_scale, us_v), (down_scale, ds_v), (gain, gain_v),
            (gate.at[0], gate_v.at[0]), (up.at[0], up_v.at[0]), (down.at[0], down_v.at[0]),
            (gate.at[1], gate_v.at[1]), (up.at[1], up_v.at[1]), (down.at[1], down_v.at[1]),
            (stream.at[pl.ds(pl.multiple_of(y * ROWS, ROWS), ROWS)], xin),
        ])
    ]
    for load in loads:
        load.start()
    for load in loads[:4]:
        load.wait()

    def put(b, m, j, tiles):
        count = tiles.shape[0] // TILE
        first, k = 8 * (j % 2), j // 2
        parts[b, first : first + count, m, TILE * k : TILE * (k + 1), :] = tiles.reshape(
            count, TILE, 128
        )

    def prepare(b):
        for m, (ref, scale) in enumerate(((gate_v, gs_v), (up_v, us_v))):
            loads[4 + 3 * b + m].wait()
            for j in range(6):
                width = 128 if j < 5 else 48
                cols = slice(128 * j, 128 * j + width)
                block = ref[b, :, cols] * scale[b : b + 1, cols]
                put(b, m, j, (block.T * gain_v[b : b + 1, :]).astype(BF16))
        loads[6 + 3 * b].wait()
        for j in range(6):
            height = 128 if j < 5 else 48
            block = down_v[b, 128 * j : 128 * j + height, :] * ds_v[b : b + 1, :]
            put(b, 2, j, block.astype(BF16))
        parts[b, 11:16, :, 2 * TILE :, :] = jnp.zeros((5, 3, TILE, 128), BF16)

    def copy(src, dst, send, recv, peer):
        return pltpu.make_async_remote_copy(
            src_ref=src, dst_ref=dst, send_sem=send, recv_sem=recv,
            device_id=peer, device_id_type=MESH,
        )

    def arrived(ref, sem):
        pltpu.make_async_copy(ref, ref, sem).wait()

    is_source = zl == own

    def spread_z(b):
        w = weights[b]

        @pl.when(is_source)
        def _():
            w[0, 0, 0] = parts[b, z]
            for quad in (2, 1, 3, 0):
                o = QUAD.index((4 - quad) % 4)
                for low in range(4):
                    if quad == 0 and low == 0:
                        continue
                    peer = at_z(quad, low)
                    copy(
                        parts.at[b, peer["ra"]], w.at[0, 0, o],
                        a_send.at[b], a_recv.at[b, o], peer,
                    ).start()

    def spread_tasks(b):
        w = weights[b]
        tasks = []

        def to_x(rel, o):
            copy(
                w.at[0, rel, o], w.at[1, rel, o], x_send.at[b], x_recv.at[b, rel, o],
                x_plus if o % 2 == 0 else x_minus,
            ).start()

        def to_y(rel, o, up_):
            there = (rel - 1) % NY if up_ else (rel + 1) % NY
            copy(
                w.at[0, rel, o], w.at[0, there, o], y_send.at[b], y_recv.at[b, there, o],
                y_plus if up_ else y_minus,
            ).start()

        def own_unit(o):
            if o == 0:
                @pl.when(jnp.logical_not(is_source))
                def _():
                    arrived(w.at[0, 0, 0], a_recv.at[b, 0])
            else:
                arrived(w.at[0, 0, o], a_recv.at[b, o])
            to_y(0, o, True)
            to_y(0, o, False)
            to_x(0, o)

        def ring_unit(s, o, up_):
            rel = (NY - s) if up_ else s
            arrived(w.at[0, rel, o], y_recv.at[b, rel, o])
            if s < 3 or (s == 3 and (o < 2) == up_):
                to_y(rel, o, up_)
            to_x(rel, o)

        def to_partner(cls, rel):
            copy(
                w.at[cls, rel], w.at[cls + 2, rel], d_send.at[b], d_recv.at[b, cls, rel], partner
            ).start()

        def own_done(rel):
            to_partner(0, rel)

        def x_done(rel):
            for o in range(4):
                arrived(w.at[1, rel, o], x_recv.at[b, rel, o])
            to_partner(1, rel)

        start = (0.0, 2.0, 2.5, 5.0)
        hop = 2.6
        for o in range(4):
            tasks.append((start[o], functools.partial(own_unit, o)))
            for s in range(1, 5):
                for up_ in (True, False):
                    if s < 4 or (o < 2) == up_:
                        tasks.append((start[o] + s * hop, functools.partial(ring_unit, s, o, up_)))
        for rel in range(NY):
            s = min(rel, NY - rel)
            tasks.append((start[3] + s * hop + 0.1, functools.partial(own_done, rel)))
            tasks.append((start[3] + (s + 1) * hop + 0.6, functools.partial(x_done, rel)))
        tasks.sort(key=lambda t: t[0])
        return [t for _, t in tasks]

    def spread_end(b):
        w = weights[b]
        for cls in range(2):
            for rel in range(NY):
                arrived(w.at[cls + 2, rel], d_recv.at[b, cls, rel])

    def source_of(cls, o):
        return 4 * ((zq + QUAD[o]) % 4) + classes[cls]

    def gather_start(b, own_rows):
        xg[b, z] = own_rows
        for k in z_peers:
            copy(
                xin if b == 0 else yb.at[0], xg.at[b, z], s_send.at[b], s_recv.at[b],
                {"ra": (z + k) % NZ},
            ).start()

    def gather_wait(b):
        arrived(xg.at[b, 0:15], s_recv.at[b])

    def hidden_of(b):
        w = weights[b]
        squares = jnp.zeros((ROWS, 128), F32)
        for i in range(NZ):
            piece = xg[b, i].astype(F32)
            squares = squares + piece * piece
        inverse = lax.rsqrt(jnp.sum(squares, axis=1, keepdims=True) / D + epsilon)
        sums = []
        for m in range(2):
            total = jnp.zeros((ROWS, 384), F32)
            for o in (0, 1, 2, 3):
                for cls in (0, 2):
                    lhs = jnp.concatenate(
                        [xg[b, source_of(cls, o)], xg[b, source_of(cls + 1, o)]], axis=1
                    )
                    rhs = jnp.concatenate(
                        [w[cls + i, :, o, m].reshape(384, 128) for i in range(2)], axis=1
                    )
                    total = total + lax.dot_general(
                        lhs, rhs, (((1,), (1,)), ((), ())), preferred_element_type=F32
                    )
            sums.append(total * inverse)
        return (sums[0] / (1.0 + jnp.exp(-sums[0])) * sums[1]).astype(BF16)

    def scatter_start(b, hidden):
        w = weights[b]
        for o in (3, 1, 2, 0):
            for cls in (0, 2):
                rhs = jnp.concatenate(
                    [w[cls + i, :, o, 2].reshape(384, 128) for i in range(2)], axis=1
                )
                piece = jnp.dot(hidden, rhs, preferred_element_type=F32).astype(BF16)
                for i in range(2):
                    ob[b, source_of(cls + i, o)] = piece[:, 128 * i : 128 * (i + 1)]
        for k in z_peers:
            there = (z + k) % NZ
            copy(ob.at[b, there], rb.at[b, z], o_send.at[b], o_recv.at[b], {"ra": there}).start()
        rb[b, z] = ob[b, z]

    def scatter_end(b, rows):
        arrived(rb.at[b, 0:15], o_recv.at[b])
        total = residual_scale * rows.astype(F32)
        for i in range(NZ):
            total = total + rb[b, i].astype(F32)
        return total.astype(BF16)

    prepare(0)
    loads[10].wait()
    pl.semaphore_wait(barrier, 25)
    spread_z(0)
    gather_start(0, xin[...])
    prepare(1)
    tasks = spread_tasks(0)
    for task in tasks[: len(tasks) // 2]:
        task()
    spread_z(1)
    for task in tasks[len(tasks) // 2 :]:
        task()
    spread_end(0)
    gather_wait(0)
    hidden = hidden_of(0)
    scatter_start(0, hidden)
    for task in spread_tasks(1):
        task()
    rows = scatter_end(0, xin[...])
    yb[0] = rows
    gather_start(1, rows)
    spread_end(1)
    gather_wait(1)
    hidden = hidden_of(1)
    scatter_start(1, hidden)
    rows = scatter_end(1, rows)
    yb[1] = rows
    final = pl.ds(pl.multiple_of(y * ROWS, ROWS), ROWS)
    out[final, :] = rows
    for k in (4, 3, 5, 2, 6, 1, 7):
        copy(
            yb.at[1], out.at[final], f_send, f_recv, {"cb": (y + k) % NY}
        ).start()
    arrived(out.at[0 : 7 * ROWS], f_recv)

    for b in range(2):
        w = weights[b]

        @pl.when(is_source)
        def _():
            arrived(parts.at[b, 0:15], a_send.at[b])

        arrived(w.at[0, 0:7], y_send.at[b])
        arrived(w.at[0], x_send.at[b])
        arrived(w.at[0:2], d_send.at[b])
        arrived(xg.at[b, 0:15], s_send.at[b])
        arrived(ob.at[b, 0:15], o_send.at[b])
    arrived(out.at[0 : 7 * ROWS], f_send)


def on_device(
    stream, norm_gain, gate_weight, up_weight, down_weight, gate_scale, up_scale, down_scale
):
    dma = pltpu.SemaphoreType.DMA
    return pl.pallas_call(
        kernel,
        out_shape=jax.ShapeDtypeStruct((256, 128), BF16),
        in_specs=[pl.BlockSpec(memory_space=pl.ANY)] * 8,
        out_specs=pl.BlockSpec(memory_space=pltpu.VMEM),
        scratch_shapes=[
            pltpu.VMEM((ROWS, 128), BF16),
            pltpu.VMEM((2, 128), F32),
            pltpu.VMEM((2, 128, 688), F32),
            pltpu.VMEM((2, 128, 688), F32),
            pltpu.VMEM((2, 688, 128), F32),
            pltpu.VMEM((2, 688), F32),
            pltpu.VMEM((2, 688), F32),
            pltpu.VMEM((2, 128), F32),
            pltpu.VMEM((2, NZ, 3, 48, 128), BF16),
            pltpu.VMEM((4, NY, 4, 3, 48, 128), BF16),
            pltpu.VMEM((4, NY, 4, 3, 48, 128), BF16),
            pltpu.VMEM((2, NZ, ROWS, 128), BF16),
            pltpu.VMEM((2, NZ, ROWS, 128), BF16),
            pltpu.VMEM((2, NZ, ROWS, 128), BF16),
            pltpu.VMEM((2, ROWS, 128), BF16),
            dma((11,)),
            dma((2,)),
            dma((2,)),
            dma((2,)),
            dma((2,)),
            dma((2, 4)),
            dma((2, NY, 4)),
            dma((2, NY, 4)),
            dma((2, 2, NY)),
            dma((2,)),
            dma((2,)),
            dma((2,)),
            dma((2,)),
            dma,
            dma,
        ],
        name="two_half_steps",
        compiler_params=pltpu.CompilerParams(
            collective_id=0, has_side_effects=True, vmem_limit_bytes=48 * 1024 * 1024
        ),
    )(stream, norm_gain, gate_weight, up_weight, down_weight, gate_scale, up_scale, down_scale)


def solution(mesh):
    in_specs = (
        P("dp", "ra"),
        P(None, "ra"),
        P(None, "ra", "cb"),
        P(None, "ra", "cb"),
        P(None, "cb", "ra"),
        P(None, "cb"),
        P(None, "cb"),
        P(None, "ra"),
    )
    out_specs = P("dp", "ra")
    return jax.shard_map(
        on_device, mesh=mesh, in_specs=in_specs, out_specs=out_specs, check_vma=False
    )
```

```python
import functools

import jax
import jax.numpy as jnp
from jax import lax
from jax.experimental import pallas as pl
from jax.experimental.pallas import tpu as pltpu
from jax.sharding import PartitionSpec as P

MESH = pl.DeviceIdType.MESH
D = 2048
epsilon = 1e-06
residual_scale = 0.5

NZ, NY = 16, 8
ROWS = 32
TILE = 16
QUAD = (0, 1, 3, 2)
RING, SKIP, FORK = {1: 0, 2: 1, 3: 2, 4: 3}, {1: 0, 2: 0, 3: 2, 4: 3}, {1: 0, 2: 0, 3: 2, 4: 2}
TREE = ((FORK, FORK, FORK, FORK), (RING, RING, RING, RING))
START = (0.0, 4.0, 4.5, 7.0)
HOP = (2.7, 3.4)
LAG = 10.0
F32, BF16 = jnp.float32, jnp.bfloat16


def kernel(
    stream, gain, gate, up, down, gate_scale, up_scale, down_scale, out,
    xin, gain_v, gate_v, up_v, down_v, gs_v, us_v, ds_v,
    parts, w0, w1, xg, ob, rb, yb,
    in_sem, a_send, y_send, x_send, d_send, a_recv, y_recv, x_recv, d_recv,
    s_send, s_recv, o_send, o_recv, f_send, f_recv,
):
    z, y, d = lax.axis_index("ra"), lax.axis_index("cb"), lax.axis_index("dp")
    zq, zl = z // 4, z % 4
    x, c = d // 2, d % 2
    p = x % 2
    own = 2 * c + p
    classes = (own, 2 * c + 1 - p, 2 * (1 - c) + p, 2 * (1 - c) + 1 - p)
    weights = (w0, w1)

    def at_z(quad, low):
        return {"ra": 4 * ((zq + quad) % 4) + (zl + low) % 4}

    far_z = sorted(
        [(k, min(k, NZ - k)) for k in range(1, NZ)], key=lambda t: -t[1]
    )
    z_peers = [k for k, _ in far_z]
    y_plus, y_minus = {"cb": (y + 1) % NY}, {"cb": (y + NY - 1) % NY}
    x_plus, x_minus = {"dp": (d + 2) % 8}, {"dp": (d + 6) % 8}
    partner = {"dp": d + 1 - 2 * c}

    barrier = pltpu.get_barrier_semaphore()
    for k in z_peers:
        pl.semaphore_signal(barrier, 1, device_id={"ra": (z + k) % NZ}, device_id_type=MESH)
    for k in (4, 3, 5, 2, 6, 1, 7):
        pl.semaphore_signal(barrier, 1, device_id={"cb": (y + k) % NY}, device_id_type=MESH)
    for peer in (x_plus, x_minus, partner):
        pl.semaphore_signal(barrier, 1, device_id=peer, device_id_type=MESH)

    loads = [
        pltpu.make_async_copy(src, dst, in_sem.at[i])
        for i, (src, dst) in enumerate([
            (gate_scale, gs_v), (up_scale, us_v), (down_scale, ds_v), (gain, gain_v),
            (gate.at[0], gate_v.at[0]), (up.at[0], up_v.at[0]), (down.at[0], down_v.at[0]),
            (gate.at[1], gate_v.at[1]), (up.at[1], up_v.at[1]), (down.at[1], down_v.at[1]),
            (stream.at[pl.ds(pl.multiple_of(y * ROWS, ROWS), ROWS)], xin),
        ])
    ]
    for load in loads:
        load.start()
    for load in loads[:4]:
        load.wait()

    def put(b, m, j, tiles):
        count = tiles.shape[0] // TILE
        first, k = 8 * (j % 2), j // 2
        parts[b, first : first + count, m, TILE * k : TILE * (k + 1), :] = tiles.reshape(
            count, TILE, 128
        )

    def prepare(b):
        for m, (ref, scale) in enumerate(((gate_v, gs_v), (up_v, us_v))):
            loads[4 + 3 * b + m].wait()
            column = scale[...].T[:, b : b + 1]
            for j in range(6):
                height = 128 if j < 5 else 48
                span = slice(128 * j, 128 * j + height)
                block = ref[b, span, :] * column[span] * gain_v[b : b + 1, :]
                put(b, m, j, block.astype(BF16))
        loads[6 + 3 * b].wait()
        for j in range(6):
            height = 128 if j < 5 else 48
            block = down_v[b, 128 * j : 128 * j + height, :] * ds_v[b : b + 1, :]
            put(b, 2, j, block.astype(BF16))
        parts[b, 11:16, :, 2 * TILE :, :] = jnp.zeros((5, 3, TILE, 128), BF16)

    def copy(src, dst, send, recv, peer):
        return pltpu.make_async_remote_copy(
            src_ref=src, dst_ref=dst, send_sem=send, recv_sem=recv,
            device_id=peer, device_id_type=MESH,
        )

    def arrived(ref, sem):
        pltpu.make_async_copy(ref, ref, sem).wait()

    is_source = zl == own

    def spread_z(b):
        w = weights[b]

        @pl.when(is_source)
        def _():
            w[0, 0, 0] = parts[b, z]
            for quad in (0, 1, 3, 2):
                o = QUAD.index((4 - quad) % 4)
                for low in range(4):
                    if quad == 0 and low == 0:
                        continue
                    peer = at_z(quad, low)
                    copy(
                        parts.at[b, peer["ra"]], w.at[0, 0, o],
                        a_send.at[b], a_recv.at[b, o], peer,
                    ).start()

    def spread_tasks(b):
        w = weights[b]
        tasks = []

        def to_x(rel, o):
            copy(
                w.at[0, rel, o], w.at[1, rel, o], x_send.at[b], x_recv.at[b, rel, o],
                x_plus if o % 2 == 0 else x_minus,
            ).start()

        def to_y(rel, o, step):
            there = (rel - step) % NY
            copy(
                w.at[0, rel, o], w.at[0, there, o], y_send.at[b], y_recv.at[b, there, o],
                {"cb": (y + step) % NY},
            ).start()

        def relay(o, offset):
            for child in reach(o):
                if parent_of(o, child) == offset:
                    to_y(-offset % NY, o, child - offset)
            to_x(-offset % NY, o)

        def reach(o):
            return (1, -1, 2, -2, 3, -3, 4 if o < 2 else -4)

        def parent_of(o, offset):
            size = TREE[b][o][abs(offset)]
            return size if offset > 0 else -size

        def own_unit(o):
            if o == 0:
                @pl.when(jnp.logical_not(is_source))
                def _():
                    arrived(w.at[0, 0, 0], a_recv.at[b, 0])
            else:
                arrived(w.at[0, 0, o], a_recv.at[b, o])
            relay(o, 0)

        def ring_unit(offset, o):
            rel = -offset % NY
            arrived(w.at[0, rel, o], y_recv.at[b, rel, o])
            relay(o, offset)

        def to_partner(cls, rel):
            copy(
                w.at[cls, rel], w.at[cls + 2, rel], d_send.at[b], d_recv.at[b, cls, rel], partner
            ).start()

        def x_done(rel):
            for o in range(4):
                arrived(w.at[1, rel, o], x_recv.at[b, rel, o])
            to_partner(1, rel)

        def time_of(o, offset):
            if offset == 0:
                return START[o]
            parent = parent_of(o, offset)
            return time_of(o, parent) + HOP[b] + 0.64 * abs(offset - parent)

        for o in range(4):
            tasks.append((time_of(o, 0), functools.partial(own_unit, o)))
            for offset in reach(o):
                tasks.append((time_of(o, offset), functools.partial(ring_unit, offset, o)))
        for rel in range(NY):
            offset = rel if rel < 4 else NY - rel
            last = max(time_of(o, offset) for o in range(4)) + 0.1
            tasks.append((last, functools.partial(to_partner, 0, rel)))
            tasks.append((last + HOP[b] + 1.0, functools.partial(x_done, rel)))
        return tasks

    def spread_end(b):
        w = weights[b]
        for cls in range(2):
            for rel in range(NY):
                arrived(w.at[cls + 2, rel], d_recv.at[b, cls, rel])

    def source_of(cls, o):
        return 4 * ((zq + QUAD[o]) % 4) + classes[cls]

    def gather_start(b, own_rows):
        xg[b, z] = own_rows
        for k in z_peers:
            copy(
                xin if b == 0 else yb.at[0], xg.at[b, z], s_send.at[b], s_recv.at[b],
                {"ra": (z + k) % NZ},
            ).start()

    def gather_wait(b):
        arrived(xg.at[b, 0:15], s_recv.at[b])

    def hidden_of(b):
        w = weights[b]
        squares = jnp.zeros((ROWS, 128), F32)
        for i in range(NZ):
            piece = xg[b, i].astype(F32)
            squares = squares + piece * piece
        inverse = lax.rsqrt(jnp.sum(squares, axis=1, keepdims=True) / D + epsilon)
        sums = []
        for m in range(2):
            total = jnp.zeros((ROWS, 384), F32)
            for o in (0, 1, 2, 3):
                for cls in (0, 2):
                    lhs = jnp.concatenate(
                        [xg[b, source_of(cls, o)], xg[b, source_of(cls + 1, o)]], axis=1
                    )
                    rhs = jnp.concatenate(
                        [w[cls + i, :, o, m].reshape(384, 128) for i in range(2)], axis=1
                    )
                    total = total + lax.dot_general(
                        lhs, rhs, (((1,), (1,)), ((), ())), preferred_element_type=F32
                    )
            sums.append(total * inverse)
        return (sums[0] / (1.0 + jnp.exp(-sums[0])) * sums[1]).astype(BF16)

    def scatter_start(b, hidden):
        w = weights[b]
        for o in (3, 1, 2, 0):
            for cls in (0, 2):
                rhs = jnp.concatenate(
                    [w[cls + i, :, o, 2].reshape(384, 128) for i in range(2)], axis=1
                )
                piece = jnp.dot(hidden, rhs, preferred_element_type=F32).astype(BF16)
                for i in range(2):
                    ob[b, source_of(cls + i, o)] = piece[:, 128 * i : 128 * (i + 1)]
        for k in z_peers:
            there = (z + k) % NZ
            copy(ob.at[b, there], rb.at[b, z], o_send.at[b], o_recv.at[b], {"ra": there}).start()
        rb[b, z] = ob[b, z]

    def scatter_end(b, rows):
        arrived(rb.at[b, 0:15], o_recv.at[b])
        total = residual_scale * rows.astype(F32)
        for i in range(NZ):
            total = total + rb[b, i].astype(F32)
        return total.astype(BF16)

    prepare(0)
    loads[10].wait()
    pl.semaphore_wait(barrier, 25)
    spread_z(0)
    gather_start(0, xin[...])
    prepare(1)
    first, second = spread_tasks(0), [(t + LAG, f) for t, f in spread_tasks(1)]
    second.append((LAG - 3.0, functools.partial(spread_z, 1)))
    ready = max(t for t, _ in first)
    rows = [None]

    def block_0():
        spread_end(0)
        gather_wait(0)
        scatter_start(0, hidden_of(0))

    def between():
        rows[0] = scatter_end(0, xin[...])
        yb[0] = rows[0]
        gather_start(1, rows[0])

    steps = first + second + [(ready + 0.1, block_0), (ready + 10.0, between)]
    for _, step in sorted(steps, key=lambda t: t[0]):
        step()
    spread_end(1)
    gather_wait(1)
    hidden = hidden_of(1)
    scatter_start(1, hidden)
    rows = scatter_end(1, rows[0])
    yb[1] = rows
    final = pl.ds(pl.multiple_of(y * ROWS, ROWS), ROWS)
    out[final, :] = rows
    for k in (4, 3, 5, 2, 6, 1, 7):
        copy(
            yb.at[1], out.at[final], f_send, f_recv, {"cb": (y + k) % NY}
        ).start()
    arrived(out.at[0 : 7 * ROWS], f_recv)

    for b in range(2):
        w = weights[b]

        @pl.when(is_source)
        def _():
            arrived(parts.at[b, 0:15], a_send.at[b])

        arrived(w.at[0, 0:7], y_send.at[b])
        arrived(w.at[0], x_send.at[b])
        arrived(w.at[0:2], d_send.at[b])
        arrived(xg.at[b, 0:15], s_send.at[b])
        arrived(ob.at[b, 0:15], o_send.at[b])
    arrived(out.at[0 : 7 * ROWS], f_send)


def on_device(
    stream, norm_gain, gate_weight, up_weight, down_weight, gate_scale, up_scale, down_scale
):
    dma = pltpu.SemaphoreType.DMA
    return pl.pallas_call(
        kernel,
        out_shape=jax.ShapeDtypeStruct((256, 128), BF16),
        in_specs=[pl.BlockSpec(memory_space=pl.ANY)] * 8,
        out_specs=pl.BlockSpec(memory_space=pltpu.VMEM),
        scratch_shapes=[
            pltpu.VMEM((ROWS, 128), BF16),
            pltpu.VMEM((2, 128), F32),
            pltpu.VMEM((2, 688, 128), F32),
            pltpu.VMEM((2, 688, 128), F32),
            pltpu.VMEM((2, 688, 128), F32),
            pltpu.VMEM((2, 688), F32),
            pltpu.VMEM((2, 688), F32),
            pltpu.VMEM((2, 128), F32),
            pltpu.VMEM((2, NZ, 3, 48, 128), BF16),
            pltpu.VMEM((4, NY, 4, 3, 48, 128), BF16),
            pltpu.VMEM((4, NY, 4, 3, 48, 128), BF16),
            pltpu.VMEM((2, NZ, ROWS, 128), BF16),
            pltpu.VMEM((2, NZ, ROWS, 128), BF16),
            pltpu.VMEM((2, NZ, ROWS, 128), BF16),
            pltpu.VMEM((2, ROWS, 128), BF16),
            dma((11,)),
            dma((2,)),
            dma((2,)),
            dma((2,)),
            dma((2,)),
            dma((2, 4)),
            dma((2, NY, 4)),
            dma((2, NY, 4)),
            dma((2, 2, NY)),
            dma((2,)),
            dma((2,)),
            dma((2,)),
            dma((2,)),
            dma,
            dma,
        ],
        name="two_half_steps",
        compiler_params=pltpu.CompilerParams(
            collective_id=0, has_side_effects=True, vmem_limit_bytes=67043328
        ),
    )(
        stream, norm_gain, jnp.swapaxes(gate_weight, 1, 2), jnp.swapaxes(up_weight, 1, 2), down_weight,
        gate_scale, up_scale, down_scale,
    )


def solution(mesh):
    in_specs = (
        P("dp", "ra"),
        P(None, "ra"),
        P(None, "ra", "cb"),
        P(None, "ra", "cb"),
        P(None, "cb", "ra"),
        P(None, "cb"),
        P(None, "cb"),
        P(None, "ra"),
    )
    out_specs = P("dp", "ra")
    return jax.shard_map(
        on_device, mesh=mesh, in_specs=in_specs, out_specs=out_specs, check_vma=False
    )
```

```python
import functools

import jax
import jax.numpy as jnp
from jax import lax
from jax.experimental import pallas as pl
from jax.experimental.pallas import tpu as pltpu
from jax.sharding import PartitionSpec as P

MESH = pl.DeviceIdType.MESH
D = 2048
epsilon = 1e-06
residual_scale = 0.5

NZ, NY = 16, 8
ROWS = 32
TILE = 16
QUAD = (0, 1, 3, 2)
RING, SKIP, FORK = {1: 0, 2: 1, 3: 2, 4: 3}, {1: 0, 2: 0, 3: 2, 4: 3}, {1: 0, 2: 0, 3: 2, 4: 2}
TREE = ((SKIP, SKIP, SKIP, FORK), (RING, RING, RING, RING))
START = ((0.0, 4.0, 4.5, 7.0), (0.0, 0.3, 0.6, 0.9))
HOP = (2.7, 3.6)
AHEAD = 3.0
NEAR, FAR = (4, 12, 3, 13, 2, 14, 1, 15), (8, 7, 9, 6, 10, 5, 11)
F32, BF16 = jnp.float32, jnp.bfloat16


def kernel(
    stream, gain, gate, up, down, gate_scale, up_scale, down_scale, out,
    xin, gain_v, gate_v, up_v, down_v, gs_v, us_v, ds_v,
    parts, w0, w1, xg, ob, rb, yb,
    in_sem, a_send, y_send, x_send, d_send, a_recv, y_recv, x_recv, d_recv,
    s_send, s_recv, o_send, o_recv, f_send, f_recv, far_sem,
):
    z, y, d = lax.axis_index("ra"), lax.axis_index("cb"), lax.axis_index("dp")
    zq, zl = z // 4, z % 4
    x, c = d // 2, d % 2
    p = x % 2
    own = 2 * c + p
    classes = (own, 2 * c + 1 - p, 2 * (1 - c) + p, 2 * (1 - c) + 1 - p)
    weights = (w0, w1)

    far_z = sorted(
        [(k, min(k, NZ - k)) for k in range(1, NZ)], key=lambda t: -t[1]
    )
    z_peers = [k for k, _ in far_z]
    y_plus, y_minus = {"cb": (y + 1) % NY}, {"cb": (y + NY - 1) % NY}
    x_plus, x_minus = {"dp": (d + 2) % 8}, {"dp": (d + 6) % 8}
    partner = {"dp": d + 1 - 2 * c}

    barrier = pltpu.get_barrier_semaphore()
    for k in NEAR:
        pl.semaphore_signal(barrier, 1, device_id={"ra": (z + k) % NZ}, device_id_type=MESH)
    for k in (4, 3, 5, 2, 6, 1, 7):
        pl.semaphore_signal(barrier, 1, device_id={"cb": (y + k) % NY}, device_id_type=MESH)
    for peer in (x_plus, x_minus, partner):
        pl.semaphore_signal(barrier, 1, device_id=peer, device_id_type=MESH)

    loads = [
        pltpu.make_async_copy(src, dst, in_sem.at[i])
        for i, (src, dst) in enumerate([
            (gate_scale, gs_v), (up_scale, us_v), (down_scale, ds_v), (gain, gain_v),
            (gate.at[0], gate_v.at[0]), (up.at[0], up_v.at[0]), (down.at[0], down_v.at[0]),
            (gate.at[1], gate_v.at[1]), (up.at[1], up_v.at[1]), (down.at[1], down_v.at[1]),
            (stream.at[pl.ds(pl.multiple_of(y * ROWS, ROWS), ROWS)], xin),
        ])
    ]
    for load in loads:
        load.start()
    for load in loads[:4]:
        load.wait()

    def put(b, m, j, tiles):
        count = tiles.shape[0] // TILE
        first, k = 8 * (j % 2), j // 2
        parts[b, first : first + count, m, TILE * k : TILE * (k + 1), :] = tiles.reshape(
            count, TILE, 128
        )

    def prepare(b):
        for m, (ref, scale) in enumerate(((gate_v, gs_v), (up_v, us_v))):
            loads[4 + 3 * b + m].wait()
            column = scale[...].T[:, b : b + 1]
            for j in range(6):
                height = 128 if j < 5 else 48
                span = slice(128 * j, 128 * j + height)
                block = ref[b, span, :] * column[span] * gain_v[b : b + 1, :]
                put(b, m, j, block.astype(BF16))
        loads[6 + 3 * b].wait()
        for j in range(6):
            height = 128 if j < 5 else 48
            block = down_v[b, 128 * j : 128 * j + height, :] * ds_v[b : b + 1, :]
            put(b, 2, j, block.astype(BF16))
        parts[b, 11:16, :, 2 * TILE :, :] = jnp.zeros((5, 3, TILE, 128), BF16)

    def copy(src, dst, send, recv, peer):
        return pltpu.make_async_remote_copy(
            src_ref=src, dst_ref=dst, send_sem=send, recv_sem=recv,
            device_id=peer, device_id_type=MESH,
        )

    def arrived(ref, sem):
        pltpu.make_async_copy(ref, ref, sem).wait()

    is_source = zl == own

    def spread_z(b, steps):
        w = weights[b]

        @pl.when(is_source)
        def _():
            if 1 in steps:
                w[0, 0, 0] = parts[b, z]
            for k in steps:
                there = (z + k) % NZ
                diff = (zq + 4 - there // 4) % 4
                o = diff + diff // 2 - 2 * (diff // 3)
                copy(
                    parts.at[b, there], w.at[0, 0, o], a_send.at[b], a_recv.at[b, o], {"ra": there}
                ).start()

    def spread_tasks(b):
        w = weights[b]
        tasks = []

        def to_x(rel, o):
            side = (o + min(rel, NY - rel) + rel // 5) % 2
            copy(
                w.at[0, rel, o], w.at[1, rel, o], x_send.at[b], x_recv.at[b, rel, o],
                x_plus if side == 0 else x_minus,
            ).start()

        def to_y(rel, o, step):
            there = (rel - step) % NY
            copy(
                w.at[0, rel, o], w.at[0, there, o], y_send.at[b], y_recv.at[b, there, o],
                {"cb": (y + step) % NY},
            ).start()

        def relay(o, offset):
            for child in reach(o):
                if parent_of(o, child) == offset:
                    to_y(-offset % NY, o, child - offset)
            to_x(-offset % NY, o)

        def reach(o):
            return (1, -1, 2, -2, 3, -3, 4 if o < 2 else -4)

        def parent_of(o, offset):
            size = TREE[b][o][abs(offset)]
            return size if offset > 0 else -size

        def own_unit(o):
            if o == 0:
                @pl.when(jnp.logical_not(is_source))
                def _():
                    arrived(w.at[0, 0, 0], a_recv.at[b, 0])
            else:
                arrived(w.at[0, 0, o], a_recv.at[b, o])
            relay(o, 0)

        def ring_unit(offset, o):
            rel = -offset % NY
            arrived(w.at[0, rel, o], y_recv.at[b, rel, o])
            relay(o, offset)

        def to_partner(cls, rel):
            copy(
                w.at[cls, rel], w.at[cls + 2, rel], d_send.at[b], d_recv.at[b, cls, rel], partner
            ).start()

        def x_done(rel):
            for o in range(4):
                arrived(w.at[1, rel, o], x_recv.at[b, rel, o])
            to_partner(1, rel)

        def time_of(o, offset):
            if offset == 0:
                return START[b][o]
            parent = parent_of(o, offset)
            return time_of(o, parent) + HOP[b] + 0.64 * abs(offset - parent)

        for o in range(4):
            tasks.append((time_of(o, 0), functools.partial(own_unit, o)))
            for offset in reach(o):
                tasks.append((time_of(o, offset), functools.partial(ring_unit, offset, o)))
        for rel in range(NY):
            offset = rel if rel < 4 else NY - rel
            last = max(time_of(o, offset) for o in range(4)) + 0.1
            tasks.append((last, functools.partial(to_partner, 0, rel)))
            tasks.append((last + HOP[b] + 1.0, functools.partial(x_done, rel)))
        return tasks

    def spread_end(b):
        w = weights[b]
        for cls in range(2):
            for rel in range(NY):
                arrived(w.at[cls + 2, rel], d_recv.at[b, cls, rel])

    def source_of(cls, o):
        return 4 * ((zq + QUAD[o]) % 4) + classes[cls]

    def gather_start(b, own_rows):
        xg[b, z] = own_rows
        for k in z_peers:
            copy(
                xin if b == 0 else yb.at[0], xg.at[b, z], s_send.at[b], s_recv.at[b],
                {"ra": (z + k) % NZ},
            ).start()

    def gather_wait(b):
        arrived(xg.at[b, 0:15], s_recv.at[b])

    def inverse_of(b):
        squares = jnp.zeros((ROWS, 128), F32)
        for i in range(NZ):
            piece = xg[b, i].astype(F32)
            squares = squares + piece * piece
        return lax.rsqrt(jnp.sum(squares, axis=1, keepdims=True) / D + epsilon)

    def sums_of(b, cls):
        w = weights[b]
        sums = []
        for m in range(2):
            total = jnp.zeros((ROWS, 384), F32)
            for o in range(4):
                lhs = jnp.concatenate(
                    [xg[b, source_of(cls, o)], xg[b, source_of(cls + 1, o)]], axis=1
                )
                rhs = jnp.concatenate(
                    [w[cls + i, :, o, m].reshape(384, 128) for i in range(2)], axis=1
                )
                total = total + lax.dot_general(
                    lhs, rhs, (((1,), (1,)), ((), ())), preferred_element_type=F32
                )
            sums.append(total)
        return sums

    def activate(sums, more, inverse):
        gate_sum, up_sum = ((a + c) * inverse for a, c in zip(sums, more))
        return (gate_sum / (1.0 + jnp.exp(-gate_sum)) * up_sum).astype(BF16)

    def scatter_start(b, hidden):
        w = weights[b]
        late = None

        def send(quad, cls):
            for i in range(2):
                there = 4 * quad + classes[cls + i]

                @pl.when(there != z)
                def _():
                    copy(
                        ob.at[b, there], rb.at[b, z], o_send.at[b], o_recv.at[b], {"ra": there}
                    ).start()

        for step in range(4):
            if b == 0:
                o = (3, 1, 2, 0)[step]
                quad = (zq + QUAD[o]) % 4
            else:
                quad = step
                diff = (quad + 4 - zq) % 4
                o = diff + diff // 2 - 2 * (diff // 3)
            for cls in (0, 2):
                rhs = jnp.concatenate(
                    [w[cls + i, :, o, 2].reshape(384, 128) for i in range(2)], axis=1
                )
                piece = jnp.dot(hidden, rhs, preferred_element_type=F32).astype(BF16)
                for i in range(2):
                    ob[b, 4 * quad + classes[cls + i]] = piece[:, 128 * i : 128 * (i + 1)]
                if late is not None:
                    send(*late)
                late = (quad, cls)
        rb[b, z] = ob[b, z]
        send(*late)

    def scatter_end(b, rows):
        arrived(rb.at[b, 0:15], o_recv.at[b])
        total = residual_scale * rows.astype(F32)
        for i in range(NZ):
            total = total + rb[b, i].astype(F32)
        return total.astype(BF16)

    prepare(0)
    loads[10].wait()
    pl.semaphore_wait(barrier, len(NEAR) + 10)
    for k in (4, 12):
        pl.semaphore_signal(far_sem, 1, device_id={"ra": (z + k) % NZ}, device_id_type=MESH)
    spread_z(0, NEAR)
    prepare(1)
    pl.semaphore_wait(far_sem, 2)
    spread_z(0, FAR)
    gather_start(0, xin[...])
    first = spread_tasks(0)
    ready = max(t for t, _ in first)
    second = [(t + ready - AHEAD, f) for t, f in spread_tasks(1)]
    second.append((5.0, functools.partial(spread_z, 1, NEAR[::-1] + FAR)))
    rows = [None]

    def block_0():
        gather_wait(0)
        inverse = inverse_of(0)
        sums = sums_of(0, 0)
        spread_end(0)
        scatter_start(0, activate(sums, sums_of(0, 2), inverse))

    def between():
        rows[0] = scatter_end(0, xin[...])
        yb[0] = rows[0]
        gather_start(1, rows[0])

    steps = first + second + [(ready + 0.1, block_0), (ready + 10.0, between)]
    for _, step in sorted(steps, key=lambda t: t[0]):
        step()
    spread_end(1)
    gather_wait(1)
    inverse = inverse_of(1)
    scatter_start(1, activate(sums_of(1, 0), sums_of(1, 2), inverse))
    rows = scatter_end(1, rows[0])
    yb[1] = rows
    final = pl.ds(pl.multiple_of(y * ROWS, ROWS), ROWS)
    out[final, :] = rows
    for k in (4, 3, 5, 2, 6, 1, 7):
        copy(
            yb.at[1], out.at[final], f_send, f_recv, {"cb": (y + k) % NY}
        ).start()
    for b in range(2):
        w = weights[b]

        @pl.when(is_source)
        def _():
            arrived(parts.at[b, 0:15], a_send.at[b])

        arrived(w.at[0, 0:7], y_send.at[b])
        arrived(w.at[0], x_send.at[b])
        arrived(w.at[0:2], d_send.at[b])
        arrived(xg.at[b, 0:15], s_send.at[b])
        arrived(ob.at[b, 0:15], o_send.at[b])
    arrived(out.at[0 : 7 * ROWS], f_recv)
    arrived(out.at[0 : 7 * ROWS], f_send)


def on_device(
    stream, norm_gain, gate_weight, up_weight, down_weight, gate_scale, up_scale, down_scale
):
    dma = pltpu.SemaphoreType.DMA
    return pl.pallas_call(
        kernel,
        out_shape=jax.ShapeDtypeStruct((256, 128), BF16),
        in_specs=[pl.BlockSpec(memory_space=pl.ANY)] * 8,
        out_specs=pl.BlockSpec(memory_space=pltpu.VMEM),
        scratch_shapes=[
            pltpu.VMEM((ROWS, 128), BF16),
            pltpu.VMEM((2, 128), F32),
            pltpu.VMEM((2, 688, 128), F32),
            pltpu.VMEM((2, 688, 128), F32),
            pltpu.VMEM((2, 688, 128), F32),
            pltpu.VMEM((2, 688), F32),
            pltpu.VMEM((2, 688), F32),
            pltpu.VMEM((2, 128), F32),
            pltpu.VMEM((2, NZ, 3, 48, 128), BF16),
            pltpu.VMEM((4, NY, 4, 3, 48, 128), BF16),
            pltpu.VMEM((4, NY, 4, 3, 48, 128), BF16),
            pltpu.VMEM((2, NZ, ROWS, 128), BF16),
            pltpu.VMEM((2, NZ, ROWS, 128), BF16),
            pltpu.VMEM((2, NZ, ROWS, 128), BF16),
            pltpu.VMEM((2, ROWS, 128), BF16),
            dma((11,)),
            dma((2,)),
            dma((2,)),
            dma((2,)),
            dma((2,)),
            dma((2, 4)),
            dma((2, NY, 4)),
            dma((2, NY, 4)),
            dma((2, 2, NY)),
            dma((2,)),
            dma((2,)),
            dma((2,)),
            dma((2,)),
            dma,
            dma,
            pltpu.SemaphoreType.REGULAR,
        ],
        name="two_half_steps",
        compiler_params=pltpu.CompilerParams(
            collective_id=0, has_side_effects=True, vmem_limit_bytes=67043328
        ),
    )(
        stream, norm_gain, jnp.swapaxes(gate_weight, 1, 2), jnp.swapaxes(up_weight, 1, 2), down_weight,
        gate_scale, up_scale, down_scale,
    )


def solution(mesh):
    in_specs = (
        P("dp", "ra"),
        P(None, "ra"),
        P(None, "ra", "cb"),
        P(None, "ra", "cb"),
        P(None, "cb", "ra"),
        P(None, "cb"),
        P(None, "cb"),
        P(None, "ra"),
    )
    out_specs = P("dp", "ra")
    return jax.shard_map(
        on_device, mesh=mesh, in_specs=in_specs, out_specs=out_specs, check_vma=False
    )
```
